32 devices in a mesh: grp: 2 (over y), tp: 4 (over z), dp: 4 (over x, core).
Axes of the slice: x: 2, y: 2, z: 4, core: 2. Of those that a mesh axis runs over, the one named last changes fastest.
Arguments:
- tokens: bfloat16 [256, 4096], P(('grp', 'tp'), 'dp'), parts along dimension 0, may hold values from -6 to 6
- lengths: int32 [64], P(('grp', 'dp')), parts along dimension 0, may hold values from 1 to 4, as said below
- norm_gain: float32 [2, 4096], P(None, 'dp'), may hold values from 0.1 to 1.9
- w_recept: bfloat16 [2, 4096, 2048], P(None, 'dp', 'tp'), may hold values from -0.09375 to 0.09375
- w_keys: bfloat16 [2, 4096, 2048], P(None, 'dp', 'tp'), may hold values from -0.09375 to 0.09375
- w_values: bfloat16 [2, 4096, 2048], P(None, 'dp', 'tp'), may hold values from -0.09375 to 0.09375
- w_decay: bfloat16 [2, 4096, 2048], P(None, 'dp', 'tp'), may hold values from -0.09375 to 0.09375
- w_rate: bfloat16 [2, 4096, 2048], P(None, 'dp', 'tp'), may hold values from -0.09375 to 0.09375
- w_gate: bfloat16 [2, 4096, 2048], P(None, 'dp', 'tp'), may hold values from -0.09375 to 0.09375
- decay_base: float32 [2, 2048], P(None, 'tp'), may hold values from -3 to 1
- group_gain: float32 [2, 2048], P(None, 'tp'), may hold values from 0.1 to 1.9
- w_out: bfloat16 [2, 2048, 4096], P(None, 'tp', 'dp'), may hold values from -0.125 to 0.125
- states: float32 [2, 64, 32, 4096], P(None, ('grp', 'dp'), 'tp'), parts along dimension 1, may hold values from -2 to 2
Outputs:
- tokens_out: bfloat16 [256, 4096], P(('grp', 'tp'), 'dp'), parts along dimension 0
- states_out: float32 [2, 64, 32, 4096], P(None, ('grp', 'dp'), 'tp'), parts along dimension 1
The draws below stay inside these ranges and needn't reach their ends.
There are 2 independent parts, one for each index of `grp`. The reference program is written for one: setup_inputs(seed, part) draws one part's arguments, and reference() takes and returns one part's arrays. A program takes and returns all parts, laid end to end along the dimension named above; an argument that names none is the same for every part. Nothing has to cross between parts.
Inputs may be any that keep to these rules, and one draw needn't show every extreme that they name: Sequence s has its first lengths[s] of its 4 slots live; in every draw all 8 sequences of some index of dp have 4 live slots.
All inputs are finite; a program needn't handle non-finite values.
Results may differ from the reference program's by a relative error of at most 0.029.
Values may be sent and summed in bfloat16 or wider, within the bound.
A program may use at most 128 MiB of HBM per device.

```python
import jax
import jax.numpy as jnp
from jax import lax

D = 4096
HEADS = 32
HEAD = 64
NEW = 4
SEQ_DEV = 8
WIDTH = 2048
SEQS = 32
TOKENS = 128


def draw_lengths(key, part):
    key_ticket = jax.random.fold_in(key, 11)
    key_block = jax.random.fold_in(key, 12)
    ticket = jax.random.randint(key_ticket, (SEQS,), 0, 100)
    length_base = 1 + (ticket >= 55).astype(jnp.int32) + (ticket >= 85).astype(jnp.int32) + (ticket >= 93).astype(jnp.int32)
    length_base = jnp.minimum(length_base, NEW)
    chosen = jax.random.randint(key_block, (), 0, SEQS // SEQ_DEV)
    owner_block = jnp.arange(SEQS, dtype=jnp.int32) // SEQ_DEV
    return jnp.where(owner_block == chosen, NEW, length_base).astype(jnp.int32)


def block_levels(key, extent, cuts, low, high):
    def one(dim, blocks):
        heights = jax.random.uniform(jax.random.fold_in(jax.random.fold_in(key, 6), dim), (blocks,), jnp.float32, low / len(cuts), high / len(cuts))
        return jnp.repeat(jnp.exp(heights), extent[dim] // blocks).reshape((-1,) + (1,) * (len(extent) - dim - 1))

    gain = one(*cuts[0])
    for cut in cuts[1:]:
        gain = gain * one(*cut)
    return gain


def scatter_about(key, shape, spread, bound, split=(), kind=jnp.bfloat16):
    drawn = spread * jax.random.normal(key, shape, jnp.float32)
    if split:
        drawn = drawn * block_levels(key, shape, split, -0.22, 0.18)
    return jnp.clip(drawn, -bound, bound).astype(kind)


def setup_inputs(seed: int = 0, part: int = 0) -> dict:
    seeds = jax.random.split(jax.random.key(seed), 14)
    part_splits = jax.random.split(jax.random.fold_in(seeds[13], part), 14)
    tokens = scatter_about(part_splits[0], (TOKENS, D), 1.0, 6.0, ((0, 4), (1, 4)))
    lengths = draw_lengths(jax.random.fold_in(jax.random.fold_in(seeds[13], part), 71), part)
    norm_gain = jnp.clip(1.0 + 0.18 * jax.random.normal(seeds[2], (2, D), jnp.float32), 0.1, 1.9)
    w_recept = scatter_about(seeds[3], (2, D, WIDTH), D ** -0.5, 0.09375, ((1, 4), (2, 4)))
    w_keys = scatter_about(seeds[4], (2, D, WIDTH), D ** -0.5, 0.09375, ((1, 4), (2, 4)))
    w_values = scatter_about(seeds[5], (2, D, WIDTH), D ** -0.5, 0.09375, ((1, 4), (2, 4)))
    w_decay = scatter_about(seeds[6], (2, D, WIDTH), D ** -0.5, 0.09375, ((1, 4), (2, 4)))
    w_rate = scatter_about(seeds[7], (2, D, WIDTH), D ** -0.5, 0.09375, ((1, 4), (2, 4)))
    w_gate = scatter_about(seeds[8], (2, D, WIDTH), D ** -0.5, 0.09375, ((1, 4), (2, 4)))
    decay_base = jnp.clip(-3.0 + 4.0 * jax.random.uniform(seeds[9], (2, WIDTH), jnp.float32) ** block_levels(seeds[9], (2, WIDTH), ((1, 4),), -0.2, 0.2), -3.0, 1.0)
    group_gain = jnp.clip(1.0 + 0.18 * jax.random.normal(seeds[10], (2, WIDTH), jnp.float32), 0.1, 1.9)
    w_out = scatter_about(seeds[11], (2, WIDTH, D), WIDTH ** -0.5, 0.125, ((1, 4), (2, 4)))
    states = scatter_about(part_splits[12], (2, SEQS, HEADS, HEAD * HEAD), 0.3, 2.0, ((1, 4), (2, 4)), jnp.float32)
    return dict(tokens=tokens, lengths=lengths, norm_gain=norm_gain, w_recept=w_recept, w_keys=w_keys, w_values=w_values, w_decay=w_decay, w_rate=w_rate, w_gate=w_gate, decay_base=decay_base, group_gain=group_gain, w_out=w_out, states=states)


norm_epsilon = 1e-06
unit_epsilon = 0.00064
group_epsilon = 0.00064

def advance(state_in, pieces, lengths, base_log, gain_vec):
    seq_count = state_in.shape[0]
    head_count = state_in.shape[1]
    head_shape = (seq_count, NEW, head_count, HEAD)
    recept, keys, values, decay_pre, rate_pre, gate_pre = [piece.astype(jnp.float32).reshape(head_shape) for piece in pieces]
    decays = jnp.exp(-jnp.exp(-jax.nn.softplus(-(base_log.reshape(head_count, HEAD) + decay_pre)) - 0.5))
    rates = jax.nn.sigmoid(rate_pre)
    unit_keys = keys * lax.rsqrt(lax.optimization_barrier(jnp.sum(keys * keys, -1, keepdims=True)) + unit_epsilon)
    memory = state_in.reshape(seq_count, head_count, HEAD, HEAD)
    live_mask = jnp.arange(NEW)[None, :] < lengths[:, None]
    readings = []
    for position in range(NEW):
        unit_now = unit_keys[:, position]
        removed = jnp.einsum('shvk,shk->shv', memory, unit_now)
        updated = memory * decays[:, position][:, :, None, :] - removed[..., None] * (unit_now * rates[:, position])[:, :, None, :] + values[:, position][..., None] * keys[:, position][:, :, None, :]
        live_now = live_mask[:, position][:, None, None, None]
        memory = jnp.where(live_now, updated, memory)
        readings.append(jnp.einsum('shvk,shk->shv', memory, recept[:, position]))
    outputs_h = jnp.stack(readings, 1)
    head_mean = lax.optimization_barrier(jnp.mean(outputs_h, -1, keepdims=True))
    head_var = lax.optimization_barrier(jnp.mean(jnp.square(outputs_h - head_mean), -1, keepdims=True))
    normed = (outputs_h - head_mean) * lax.rsqrt(head_var + group_epsilon) * gain_vec.reshape(head_count, HEAD)
    mixed_out = normed * jax.nn.sigmoid(gate_pre) * live_mask[:, :, None, None].astype(jnp.float32)
    return (memory.reshape(state_in.shape), mixed_out.reshape(seq_count * NEW, head_count * HEAD).astype(jnp.bfloat16))

def reference(tokens, lengths, norm_gain, w_recept, w_keys, w_values, w_decay, w_rate, w_gate, decay_base, group_gain, w_out, states):
    current = tokens
    new_states = []
    for layer_id in range(2):
        wide_rows = current.astype(jnp.float32)
        inv_rms = lax.rsqrt(lax.optimization_barrier(jnp.sum(wide_rows * wide_rows, -1, keepdims=True)) / D + norm_epsilon)
        scaled = (wide_rows * norm_gain[layer_id]).astype(jnp.bfloat16)
        pieces = [(inv_rms * jnp.dot(scaled, matrix[layer_id], preferred_element_type=jnp.float32)).astype(jnp.bfloat16) for matrix in (w_recept, w_keys, w_values, w_decay, w_rate, w_gate)]
        memory, mixed_out = advance(states[layer_id], pieces, lengths, decay_base[layer_id], group_gain[layer_id])
        new_states.append(memory)
        current = (wide_rows + jnp.dot(mixed_out, w_out[layer_id], preferred_element_type=jnp.float32)).astype(jnp.bfloat16)
    return (current, jnp.stack(new_states))
```

```python
import functools

import jax
import jax.numpy as jnp
from jax import lax
from jax.experimental import pallas as pl
from jax.experimental.pallas import tpu as pltpu
from jax.sharding import PartitionSpec as P

HEAD = 64
LANES = 2 * HEAD
NEW = 4
ROLES = 6
norm_epsilon = 1e-06
unit_epsilon = 0.00064
group_epsilon = 0.00064
MESH = pl.DeviceIdType.MESH
f32 = jnp.float32
bf16 = jnp.bfloat16


def kernel(
    tp_n,
    dp_n,
    model_width,
    tokens,
    lengths,
    norm_gain,
    w_recept,
    w_keys,
    w_values,
    w_decay,
    w_rate,
    w_gate,
    decay_base,
    group_gain,
    w_out,
    states,
    tokens_out,
    states_out,
    gat,
    gain_vm,
    base_vm,
    group_vm,
    w_vm,
    wo_vm,
    st_vm,
    so_vm,
    expand,
    scaled,
    part,
    pair,
    csend,
    crecv,
    sq_part,
    sq_pair,
    sq_send,
    sq_recv,
    yscr,
    rel,
    rows_base,
    rows_gain,
    rows_len,
    prod,
    mixrel,
    mixf,
    mixed,
    psend,
    precv,
    ship,
    load_sem,
    w_sem,
    store_sem,
    gat_s,
    gat_r,
    pair_s,
    pair_r,
    cs_s,
    cs_r,
    mix_s,
    mix_r,
    p_s,
    p_r,
):
    g = lax.axis_index("grp")
    t = lax.axis_index("tp")
    d = lax.axis_index("dp")
    chips = dp_n // 2
    x = d // 2
    c = lax.rem(d, 2)
    local, feat = tokens.shape
    total = local * tp_n
    own = total // dp_n
    width = w_recept.shape[2]
    heads = width // HEAD
    seqs = own // NEW
    rows = seqs * heads
    flat = states.shape[2]

    own_gat = gat.at[0, pl.ds(pl.multiple_of(t * local, local), local)]
    loads = [
        pltpu.make_async_copy(tokens, own_gat, load_sem.at[0]),
        pltpu.make_async_copy(norm_gain, gain_vm, load_sem.at[1]),
        pltpu.make_async_copy(decay_base, base_vm, load_sem.at[2]),
        pltpu.make_async_copy(group_gain, group_vm, load_sem.at[3]),
    ]
    for copy in loads:
        copy.start()
    weights = (w_recept, w_keys, w_values, w_decay, w_rate, w_gate)
    w_loads, wo_loads, st_loads = [], [], []
    for b in range(2):
        w_loads.append(
            [
                pltpu.make_async_copy(weights[r].at[b], w_vm.at[b, r], w_sem.at[b, r])
                for r in range(ROLES)
            ]
        )
        st_loads.append(pltpu.make_async_copy(states.at[b], st_vm.at[b], w_sem.at[b, ROLES]))
        wo_loads.append(pltpu.make_async_copy(w_out.at[b], wo_vm.at[b], w_sem.at[b, ROLES + 1]))
        for copy in w_loads[b]:
            copy.start()
        st_loads[b].start()
        wo_loads[b].start()

    def tp_peer(o):
        return (g, lax.rem(t + o, tp_n), d)

    def dp_peer(o):
        return (g, t, lax.rem(d + o, dp_n))

    sibling = (g, t, x * 2 + 1 - c)

    def chip_peer(o):
        return (g, t, lax.rem(x + o, chips) * 2 + c)

    barrier = pltpu.get_barrier_semaphore()
    for o in range(1, tp_n):
        pl.semaphore_signal(barrier, inc=1, device_id=tp_peer(o), device_id_type=MESH)
    for o in range(1, dp_n):
        pl.semaphore_signal(barrier, inc=1, device_id=dp_peer(o), device_id_type=MESH)
    pl.semaphore_wait(barrier, tp_n - 1 + dp_n - 1)

    def remote(src, dst, ss, rs, dev):
        return pltpu.make_async_remote_copy(
            src_ref=src, dst_ref=dst, send_sem=ss, recv_sem=rs, device_id=dev, device_id_type=MESH
        )

    pending = []

    def gather_tokens(b):
        mine = gat.at[b, pl.ds(pl.multiple_of(t * local, local), local)]
        copies = [
            remote(mine, mine, gat_s.at[b, o], gat_r.at[b, o], tp_peer(o)) for o in range(1, tp_n)
        ]
        for copy in copies:
            copy.start()
        pending.extend(copies)
        return copies

    loads[0].wait()
    arrivals = gather_tokens(0)
    for copy in loads[1:]:
        copy.wait()

    lane = lax.broadcasted_iota(jnp.int32, (seqs, LANES), 1)
    low = lane < HEAD

    chunk = 512
    for i in range(flat // chunk):
        r_id = lax.broadcasted_iota(jnp.int32, (chunk, LANES), 0) + i * chunk
        c_id = lax.broadcasted_iota(jnp.int32, (chunk, LANES), 1)
        expand[pl.ds(i * chunk, chunk), :] = jnp.where(
            (r_id // HEAD) == lax.rem(c_id, HEAD), 1.0, 0.0
        ).astype(bf16)
    for b in range(2):
        for src, dst in ((base_vm, rows_base), (group_vm, rows_gain)):
            for hp in range(heads // 2):
                a = jnp.broadcast_to(src[b : b + 1, hp * LANES : (hp + 1) * LANES], (seqs, LANES))
                turned = pltpu.roll(a, HEAD, 1)
                dst[b, pl.ds(2 * hp, seqs, stride=heads), :] = jnp.where(low, a, turned)
                dst[b, pl.ds(2 * hp + 1, seqs, stride=heads), :] = jnp.where(low, turned, a)
    for s in range(seqs):
        rows_len[s * heads : (s + 1) * heads, :] = jnp.full(
            (heads, LANES), lengths[s].astype(f32), f32
        )

    for b in range(2):
        for copy in arrivals:
            copy.wait_recv()
        wide = gat[b].astype(f32)
        scaled[...] = (wide * gain_vm[b : b + 1, :]).astype(bf16)
        square = jnp.broadcast_to(jnp.sum(wide * wide, 1, keepdims=True), (total, LANES))
        sq_part[b] = square.reshape(chips, 2, own, LANES)

        def to_sibling(src, dst, i):
            copy = remote(
                src.at[:, 1 - c], dst, pair_s.at[b, i], pair_r.at[b, i], sibling
            )
            copy.start()
            pending.append(copy)
            return copy

        def to_chips(src, dst, i):
            copies = []
            for o in range(1, chips):
                copy = remote(
                    src.at[lax.rem(x + o, chips)],
                    dst.at[o],
                    cs_s.at[b, i, o],
                    cs_r.at[b, i, o],
                    chip_peer(o),
                )
                copy.start()
                copies.append(copy)
            pending.extend(copies)
            return copies

        pair_copies = [to_sibling(sq_part.at[b], sq_pair.at[b], ROLES)]
        chip_copies = []

        def forward_square():
            pair_copies[0].wait_recv()
            for o in range(1, chips):
                xx = lax.rem(x + o, chips)
                sq_send[b, xx] = sq_part[b, xx, c] + sq_pair[b, xx]
            chip_copies.append(to_chips(sq_send.at[b], sq_recv.at[b], ROLES))

        def forward(r):
            pair_copies[r + 1].wait_recv()
            for o in range(1, chips):
                xx = lax.rem(x + o, chips)
                csend[b, r, xx] = (
                    part[b, r, xx, c].astype(f32) + pair[b, r, xx].astype(f32)
                ).astype(bf16)
            chip_copies.append(to_chips(csend.at[b, r], crecv.at[b, r], r))

        for r in range(ROLES):
            w_loads[b][r].wait()
            y = jnp.dot(scaled[...], w_vm[b, r], preferred_element_type=f32)
            part[b, r] = y.astype(bf16).reshape(chips, 2, own, width)
            pair_copies.append(to_sibling(part.at[b, r], pair.at[b, r], r))
            if r == 0:
                forward_square()
            else:
                forward(r - 1)
        forward(ROLES - 1)

        for copy in chip_copies[0]:
            copy.wait_recv()
        square = sq_part[b, x, c] + sq_pair[b, x]
        for o in range(1, chips):
            square = square + sq_recv[b, o]
        inv_rms = lax.rsqrt(square[:, :1] / model_width + norm_epsilon)

        for r in range(ROLES):
            for copy in chip_copies[r + 1]:
                copy.wait_recv()
            y = part[b, r, x, c].astype(f32) + pair[b, r, x].astype(f32)
            for o in range(1, chips):
                y = y + crecv[b, r, o].astype(f32)
            y = (inv_rms * y).astype(bf16).astype(f32)
            for hp in range(heads // 2):
                yscr[r, hp] = y[:, hp * LANES : (hp + 1) * LANES]
            for n in range(NEW):
                for hp in range(heads // 2):
                    a = yscr[r, hp, pl.ds(n, seqs, stride=NEW), :]
                    turned = pltpu.roll(a, HEAD, 1)
                    rel[r * NEW + n, pl.ds(2 * hp, seqs, stride=heads), :] = jnp.where(
                        low, a, turned
                    )
                    rel[r * NEW + n, pl.ds(2 * hp + 1, seqs, stride=heads), :] = jnp.where(
                        low, turned, a
                    )

        def half_sum(z):
            return 0.5 * jnp.sum(z, 1, keepdims=True)

        st_loads[b].wait()
        carried = None
        units, cs, ks, qs, vs, ws, vecs_u, vecs_q, lives = [], [], [], [], [], [], [], [], []
        for n in range(NEW):
            q, k, v, dec, rate = [rel[r * NEW + n] for r in range(5)]
            live = jnp.where(rows_len[...] > n + 0.5, 1.0, 0.0)
            w = jnp.exp(-jnp.exp(-jax.nn.softplus(-(rows_base[b] + dec)) - 0.5))
            w = jnp.where(live > 0.5, w, 1.0)
            u = k * lax.rsqrt(half_sum(k * k) + unit_epsilon)
            units.append(u)
            cs.append(live * (u * jax.nn.sigmoid(rate)))
            ks.append(live * k)
            qs.append(q)
            vs.append(v)
            ws.append(w)
            lives.append(live)
            vecs_u.append(u if carried is None else carried * u)
            carried = w if carried is None else carried * w
            vecs_q.append(carried * q)
        for j in range(flat // LANES):
            s0 = st_vm[b, :, j * LANES : (j + 1) * LANES]
            for i, vec in enumerate(vecs_u + vecs_q):
                prod[i * rows : (i + 1) * rows, j * LANES : (j + 1) * LANES] = (s0 * vec).astype(
                    bf16
                )
        reads = jnp.dot(prod[...], expand[...], preferred_element_type=f32)
        ps, ct, kt = [], [], []
        for n in range(NEW):
            p = reads[n * rows : (n + 1) * rows]
            for j in range(n):
                p = p - ps[j] * half_sum(ct[j] * units[n]) + vs[j] * half_sum(kt[j] * units[n])
            ps.append(p)
            ct = [z * ws[n] for z in ct] + [cs[n]]
            kt = [z * ws[n] for z in kt] + [ks[n]]
            o_n = reads[(NEW + n) * rows : (NEW + n + 1) * rows]
            for j in range(n + 1):
                o_n = o_n - ps[j] * half_sum(ct[j] * qs[n]) + vs[j] * half_sum(kt[j] * qs[n])
            mean = jnp.mean(o_n, 1, keepdims=True)
            off = o_n - mean
            var = jnp.mean(off * off, 1, keepdims=True)
            normed = off * lax.rsqrt(var + group_epsilon) * rows_gain[b]
            mixrel[n] = lives[n] * jax.nn.sigmoid(rel[5 * NEW + n]) * normed
            for hp in range(heads // 2):
                even = mixrel[n, pl.ds(2 * hp, seqs, stride=heads), :]
                odd = mixrel[n, pl.ds(2 * hp + 1, seqs, stride=heads), :]
                mixf[hp, pl.ds(n, seqs, stride=NEW), :] = jnp.where(low, even, odd)
        for hp in range(heads // 2):
            mixed[
                b, pl.ds(pl.multiple_of(d * own, own), own), hp * LANES : (hp + 1) * LANES
            ] = mixf[hp].astype(bf16)
        mine = mixed.at[b, pl.ds(pl.multiple_of(d * own, own), own)]
        mix_copies = [
            remote(mine, mine, mix_s.at[b, o], mix_r.at[b, o], dp_peer(o)) for o in range(1, dp_n)
        ]
        for copy in mix_copies:
            copy.start()
        pending.extend(mix_copies)

        wide_lane = lax.broadcasted_iota(jnp.int32, (rows, LANES), 1) < HEAD
        for i in range(NEW):
            ship[2 * i * rows : (2 * i + 1) * rows, :] = jnp.where(wide_lane, -ps[i], 0.0).astype(
                bf16
            )
            ship[(2 * i + 1) * rows : (2 * i + 2) * rows, :] = jnp.where(
                wide_lane, vs[i], 0.0
            ).astype(bf16)
        step = 512
        for j in range(flat // step):
            spread = lax.dot_general(
                ship[...],
                expand[j * step : (j + 1) * step, :],
                (((1,), (1,)), ((), ())),
                preferred_element_type=f32,
            )
            for m in range(step // LANES):
                lanes = slice(m * LANES, (m + 1) * LANES)
                at = slice(j * step + m * LANES, j * step + (m + 1) * LANES)
                acc = st_vm[b, :, at] * carried
                for i in range(NEW):
                    acc = acc + spread[2 * i * rows : (2 * i + 1) * rows, lanes] * ct[i]
                    acc = acc + spread[(2 * i + 1) * rows : (2 * i + 2) * rows, lanes] * kt[i]
                so_vm[b, :, at] = acc
        pltpu.make_async_copy(so_vm.at[b], states_out.at[b], store_sem.at[b]).start()

        for copy in mix_copies:
            copy.wait_recv()
        wo_loads[b].wait()
        outp = jnp.dot(mixed[b], wo_vm[b], preferred_element_type=f32)
        psend[b] = outp.astype(bf16).reshape(tp_n, local, feat)
        p_copies = []
        for o in range(1, tp_n):
            copy = remote(
                psend.at[b, lax.rem(t + o, tp_n)],
                precv.at[b, o],
                p_s.at[b, o],
                p_r.at[b, o],
                tp_peer(o),
            )
            copy.start()
            p_copies.append(copy)
        pending.extend(p_copies)
        here = pl.ds(pl.multiple_of(t * local, local), local)
        acc = psend[b, t].astype(f32)
        for o in range(1, tp_n):
            p_copies[o - 1].wait_recv()
            acc = acc + precv[b, o].astype(f32)
        fresh = (gat[b, here, :].astype(f32) + acc).astype(bf16)
        if b == 0:
            gat[1, here, :] = fresh
            arrivals = gather_tokens(1)
        else:
            tokens_out[...] = fresh

    for b in range(2):
        pltpu.make_async_copy(so_vm.at[b], states_out.at[b], store_sem.at[b]).wait()
    for copy in pending:
        copy.wait_send()


def solution(mesh):
    tp_n = mesh.shape["tp"]
    dp_n = mesh.shape["dp"]
    chips = dp_n // 2

    def per_device(*args):
        tokens, lengths = args[0], args[1]
        w_recept, w_out, states = args[3], args[11], args[12]
        local, feat = tokens.shape
        total = local * tp_n
        own = total // dp_n
        width = w_recept.shape[2]
        heads = width // HEAD
        seqs = lengths.shape[0]
        rows = seqs * heads
        flat = states.shape[3]
        flat_states = states.reshape(2, rows, flat)
        any_spec = pl.BlockSpec(memory_space=pl.ANY)
        vmem = pltpu.VMEM
        dma = pltpu.SemaphoreType.DMA
        tokens_out, states_out = pl.pallas_call(
            functools.partial(kernel, tp_n, dp_n, feat * dp_n),
            out_shape=(
                jax.ShapeDtypeStruct((local, feat), bf16),
                jax.ShapeDtypeStruct((2, rows, flat), f32),
            ),
            in_specs=[any_spec, pl.BlockSpec(memory_space=pltpu.SMEM)] + [any_spec] * 11,
            out_specs=(pl.BlockSpec(memory_space=pltpu.VMEM), any_spec),
            scratch_shapes=[
                vmem((2, total, feat), bf16),
                vmem((2, feat), f32),
                vmem((2, width), f32),
                vmem((2, width), f32),
                vmem((2, ROLES, feat, width), bf16),
                vmem((2, width, feat), bf16),
                vmem((2, rows, flat), f32),
                vmem((2, rows, flat), f32),
                vmem((flat, LANES), bf16),
                vmem((total, feat), bf16),
                vmem((2, ROLES, chips, 2, own, width), bf16),
                vmem((2, ROLES, chips, own, width), bf16),
                vmem((2, ROLES, chips, own, width), bf16),
                vmem((2, ROLES, chips, own, width), bf16),
                vmem((2, chips, 2, own, LANES), f32),
                vmem((2, chips, own, LANES), f32),
                vmem((2, chips, own, LANES), f32),
                vmem((2, chips, own, LANES), f32),
                vmem((ROLES, heads // 2, own, LANES), f32),
                vmem((ROLES * NEW, rows, LANES), f32),
                vmem((2, rows, LANES), f32),
                vmem((2, rows, LANES), f32),
                vmem((rows, LANES), f32),
                vmem((2 * NEW * rows, flat), bf16),
                vmem((NEW, rows, LANES), f32),
                vmem((heads // 2, own, LANES), f32),
                vmem((2, total, width), bf16),
                vmem((2, tp_n, local, feat), bf16),
                vmem((2, tp_n, local, feat), bf16),
                vmem((2 * NEW * rows, LANES), bf16),
                dma((4,)),
                dma((2, ROLES + 2)),
                dma((2,)),
                dma((2, tp_n)),
                dma((2, tp_n)),
                dma((2, ROLES + 1)),
                dma((2, ROLES + 1)),
                dma((2, ROLES + 1, chips)),
                dma((2, ROLES + 1, chips)),
                dma((2, dp_n)),
                dma((2, dp_n)),
                dma((2, tp_n)),
                dma((2, tp_n)),
            ],
            compiler_params=pltpu.CompilerParams(
                collective_id=0, has_side_effects=True, vmem_limit_bytes=60 * 1024 * 1024
            ),
        )(*args[:12], flat_states)
        return tokens_out, states_out.reshape(states.shape)

    placed = (
        P(("grp", "tp"), "dp"),
        P(("grp", "dp")),
        P(None, "dp"),
        P(None, "dp", "tp"),
        P(None, "dp", "tp"),
        P(None, "dp", "tp"),
        P(None, "dp", "tp"),
        P(None, "dp", "tp"),
        P(None, "dp", "tp"),
        P(None, "tp"),
        P(None, "tp"),
        P(None, "tp", "dp"),
        P(None, ("grp", "dp"), "tp", None),
    )
    return jax.shard_map(
        per_device,
        mesh=mesh,
        in_specs=placed,
        out_specs=(P(("grp", "tp"), "dp"), P(None, ("grp", "dp"), "tp", None)),
        check_vma=False,
    )
```

```python
import functools

import jax
import jax.numpy as jnp
from jax import lax
from jax.experimental import pallas as pl
from jax.experimental.pallas import tpu as pltpu
from jax.sharding import PartitionSpec as P

HEAD = 64
LANES = 2 * HEAD
NEW = 4
ROLES = 6
norm_epsilon = 1e-06
unit_epsilon = 0.00064
group_epsilon = 0.00064
MESH = pl.DeviceIdType.MESH
f32 = jnp.float32
bf16 = jnp.bfloat16


def kernel(
    tp_n,
    dp_n,
    model_width,
    tokens,
    lengths,
    norm_gain,
    w_recept,
    w_keys,
    w_values,
    w_decay,
    w_rate,
    w_gate,
    decay_base,
    group_gain,
    w_out,
    states,
    tokens_out,
    states_out,
    gat,
    gain_vm,
    base_vm,
    group_vm,
    w_vm,
    wo_vm,
    st_vm,
    so_vm,
    expand,
    scaled,
    part,
    pair,
    csend,
    crecv,
    sq_part,
    sq_pair,
    sq_send,
    sq_recv,
    yscr,
    rel,
    rows_base,
    rows_gain,
    rows_len,
    prod,
    mixrel,
    mixf,
    mixed,
    psend,
    precv,
    ship,
    factors,
    run,
    came,
    run_s,
    run_r,
    load_sem,
    w_sem,
    store_sem,
    gat_s,
    gat_r,
    pair_s,
    pair_r,
    cs_s,
    cs_r,
    mix_s,
    mix_r,
    p_s,
    p_r,
):
    g = lax.axis_index("grp")
    t = lax.axis_index("tp")
    d = lax.axis_index("dp")
    chips = dp_n // 2
    x = d // 2
    c = lax.rem(d, 2)
    local, feat = tokens.shape
    total = local * tp_n
    own = total // dp_n
    width = w_recept.shape[2]
    heads = width // HEAD
    seqs = own // NEW
    rows = seqs * heads
    flat = states.shape[2]

    own_gat = gat.at[0, pl.ds(pl.multiple_of(t * local, local), local)]
    loads = [
        pltpu.make_async_copy(tokens, own_gat, load_sem.at[0]),
        pltpu.make_async_copy(norm_gain, gain_vm, load_sem.at[1]),
        pltpu.make_async_copy(decay_base, base_vm, load_sem.at[2]),
        pltpu.make_async_copy(group_gain, group_vm, load_sem.at[3]),
    ]
    for copy in loads:
        copy.start()
    weights = (w_keys, w_decay, w_recept, w_rate, w_values, w_gate)
    w_loads, wo_loads, st_loads = [], [], []
    for b in range(2):
        w_loads.append(
            [
                pltpu.make_async_copy(weights[r].at[b], w_vm.at[b, r], w_sem.at[b, r])
                for r in range(ROLES)
            ]
        )
        st_loads.append(pltpu.make_async_copy(states.at[b], st_vm.at[b], w_sem.at[b, ROLES]))
        wo_loads.append(pltpu.make_async_copy(w_out.at[b], wo_vm.at[b], w_sem.at[b, ROLES + 1]))
        for copy in w_loads[b]:
            copy.start()
        st_loads[b].start()
        wo_loads[b].start()

    def tp_peer(o):
        return (g, lax.rem(t + o, tp_n), d)

    def dp_peer(o):
        return (g, t, lax.rem(d + o, dp_n))

    sibling = (g, t, x * 2 + 1 - c)

    def chip_peer(o):
        return (g, t, lax.rem(x + o, chips) * 2 + c)

    barrier = pltpu.get_barrier_semaphore()
    for o in range(1, tp_n):
        pl.semaphore_signal(barrier, inc=1, device_id=tp_peer(o), device_id_type=MESH)
    for o in range(1, dp_n):
        pl.semaphore_signal(barrier, inc=1, device_id=dp_peer(o), device_id_type=MESH)
    pl.semaphore_wait(barrier, tp_n - 1 + dp_n - 1)

    def remote(src, dst, ss, rs, dev):
        return pltpu.make_async_remote_copy(
            src_ref=src, dst_ref=dst, send_sem=ss, recv_sem=rs, device_id=dev, device_id_type=MESH
        )

    pending = []

    def gather_tokens(b):
        mine = gat.at[b, pl.ds(pl.multiple_of(t * local, local), local)]
        copies = [
            remote(mine, mine, gat_s.at[b, o], gat_r.at[b, o], tp_peer(o)) for o in range(1, tp_n)
        ]
        for copy in copies:
            copy.start()
        pending.extend(copies)
        return copies

    loads[0].wait()
    arrivals = gather_tokens(0)
    for copy in loads[1:]:
        copy.wait()

    lane = lax.broadcasted_iota(jnp.int32, (seqs, LANES), 1)
    low = lane < HEAD

    chunk = 512
    for i in range(flat // chunk):
        r_id = lax.broadcasted_iota(jnp.int32, (chunk, LANES), 0) + i * chunk
        c_id = lax.broadcasted_iota(jnp.int32, (chunk, LANES), 1)
        expand[pl.ds(i * chunk, chunk), :] = jnp.where(
            (r_id // HEAD) == lax.rem(c_id, HEAD), 1.0, 0.0
        ).astype(bf16)
    for b in range(2):
        for src, dst in ((base_vm, rows_base), (group_vm, rows_gain)):
            for hp in range(heads // 2):
                a = jnp.broadcast_to(src[b : b + 1, hp * LANES : (hp + 1) * LANES], (seqs, LANES))
                turned = pltpu.roll(a, HEAD, 1)
                dst[b, pl.ds(2 * hp, seqs, stride=heads), :] = jnp.where(low, a, turned)
                dst[b, pl.ds(2 * hp + 1, seqs, stride=heads), :] = jnp.where(low, turned, a)
    for s in range(seqs):
        rows_len[s * heads : (s + 1) * heads, :] = jnp.full(
            (heads, LANES), lengths[s].astype(f32), f32
        )

    half = local // 2
    step = 512
    early = (3, 3)

    @pl.when(t == 0)
    def _():
        came[0] = jnp.zeros(came.shape[1:], bf16)

    @pl.when(t == tp_n - 1)
    def _():
        came[1] = jnp.zeros(came.shape[1:], bf16)

    def half_sum(z):
        return 0.5 * jnp.sum(z, 1, keepdims=True)

    def new_state(b, start, stop):
        for j in range(start, stop):
            spread = lax.dot_general(
                ship[b],
                expand[j * step : (j + 1) * step, :],
                (((1,), (1,)), ((), ())),
                preferred_element_type=f32,
            )
            for m in range(step // LANES):
                lanes = slice(m * LANES, (m + 1) * LANES)
                at = slice(j * step + m * LANES, j * step + (m + 1) * LANES)
                acc = st_vm[b, :, at] * factors[b, 0]
                for i in range(NEW):
                    acc = (
                        acc
                        + spread[2 * i * rows : (2 * i + 1) * rows, lanes] * factors[b, 1 + i]
                        + spread[(2 * i + 1) * rows : (2 * i + 2) * rows, lanes]
                        * factors[b, 1 + NEW + i]
                    )
                so_vm[b, :, at] = acc
        if stop == flat // step:
            pltpu.make_async_copy(so_vm.at[b], states_out.at[b], store_sem.at[b]).start()

    for b in range(2):
        if b == 0:
            for copy in arrivals:
                copy.wait_recv()
        wide = gat[b].astype(f32)
        scaled[...] = (wide * gain_vm[b : b + 1, :]).astype(bf16)
        square = jnp.broadcast_to(jnp.sum(wide * wide, 1, keepdims=True), (total, LANES))
        sq_part[b] = square.reshape(chips, 2, own, LANES)

        def to_sibling(src, dst, i):
            copy = remote(
                src.at[:, 1 - c], dst, pair_s.at[b, i], pair_r.at[b, i], sibling
            )
            copy.start()
            pending.append(copy)
            return copy

        def to_chips(src, dst, i):
            copies = []
            for o in range(1, chips):
                copy = remote(
                    src.at[lax.rem(x + o, chips)],
                    dst.at[o],
                    cs_s.at[b, i, o],
                    cs_r.at[b, i, o],
                    chip_peer(o),
                )
                copy.start()
                copies.append(copy)
            pending.extend(copies)
            return copies

        pair_copies = [to_sibling(sq_part.at[b], sq_pair.at[b], ROLES)]
        chip_copies = []

        def forward_square():
            pair_copies[0].wait_recv()
            for o in range(1, chips):
                xx = lax.rem(x + o, chips)
                sq_send[b, xx] = sq_part[b, xx, c] + sq_pair[b, xx]
            chip_copies.append(to_chips(sq_send.at[b], sq_recv.at[b], ROLES))

        def forward(r):
            pair_copies[r + 1].wait_recv()
            for o in range(1, chips):
                xx = lax.rem(x + o, chips)
                csend[b, r, xx] = (
                    part[b, r, xx, c].astype(f32) + pair[b, r, xx].astype(f32)
                ).astype(bf16)
            chip_copies.append(to_chips(csend.at[b, r], crecv.at[b, r], r))

        for r in range(ROLES):
            w_loads[b][r].wait()
            y = jnp.dot(scaled[...], w_vm[b, r], preferred_element_type=f32)
            part[b, r] = y.astype(bf16).reshape(chips, 2, own, width)
            pair_copies.append(to_sibling(part.at[b, r], pair.at[b, r], r))
            if r == 0:
                forward_square()
            else:
                forward(r - 1)
        forward(ROLES - 1)

        for copy in chip_copies[0]:
            copy.wait_recv()
        square = sq_part[b, x, c] + sq_pair[b, x]
        for o in range(1, chips):
            square = square + sq_recv[b, o]
        inv_rms = lax.rsqrt(square[:, :1] / model_width + norm_epsilon)

        def receive(r):
            for copy in chip_copies[r + 1]:
                copy.wait_recv()
            y = part[b, r, x, c].astype(f32) + pair[b, r, x].astype(f32)
            for o in range(1, chips):
                y = y + crecv[b, r, o].astype(f32)
            y = (inv_rms * y).astype(bf16).astype(f32)
            for hp in range(heads // 2):
                yscr[r, hp] = y[:, hp * LANES : (hp + 1) * LANES]
            for n in range(NEW):
                for hp in range(heads // 2):
                    a = yscr[r, hp, pl.ds(n, seqs, stride=NEW), :]
                    turned = pltpu.roll(a, HEAD, 1)
                    rel[r * NEW + n, pl.ds(2 * hp, seqs, stride=heads), :] = jnp.where(
                        low, a, turned
                    )
                    rel[r * NEW + n, pl.ds(2 * hp + 1, seqs, stride=heads), :] = jnp.where(
                        low, turned, a
                    )
            return [rel[r * NEW + n] for n in range(NEW)]

        def read_state(vecs):
            for j in range(flat // LANES):
                s0 = st_vm[b, :, j * LANES : (j + 1) * LANES]
                for i, vec in enumerate(vecs):
                    prod[i * rows : (i + 1) * rows, j * LANES : (j + 1) * LANES] = (
                        s0 * vec
                    ).astype(bf16)
            return jnp.dot(prod[...], expand[...], preferred_element_type=f32)

        st_loads[b].wait()
        keys = receive(0)
        decs = receive(1)
        lives, ws, units, ks, vecs, carry = [], [], [], [], [], []
        carried = None
        for n in range(NEW):
            live = jnp.where(rows_len[...] > n + 0.5, 1.0, 0.0)
            w = jnp.exp(-jnp.exp(-jax.nn.softplus(-(rows_base[b] + decs[n])) - 0.5))
            w = jnp.where(live > 0.5, w, 1.0)
            k = keys[n]
            u = k * lax.rsqrt(half_sum(k * k) + unit_epsilon)
            lives.append(live)
            units.append(u)
            ks.append(live * k)
            ws.append(w)
            vecs.append(u if carried is None else carried * u)
            carried = w if carried is None else carried * w
            carry.append(carried)
        reads_u = read_state(vecs)
        qs = receive(2)
        reads_q = read_state([carry[n] * qs[n] for n in range(NEW)])
        rates = receive(3)
        cs = [lives[n] * (units[n] * jax.nn.sigmoid(rates[n])) for n in range(NEW)]
        ct, kt, u_c, u_k, q_c, q_k = [], [], [], [], [], []
        for n in range(NEW):
            u_c.append([half_sum(z * units[n]) for z in ct])
            u_k.append([half_sum(z * units[n]) for z in kt])
            ct = [z * ws[n] for z in ct] + [cs[n]]
            kt = [z * ws[n] for z in kt] + [ks[n]]
            q_c.append([half_sum(z * qs[n]) for z in ct])
            q_k.append([half_sum(z * qs[n]) for z in kt])
        factors[b, 0] = carried
        for n in range(NEW):
            factors[b, 1 + n] = ct[n]
            factors[b, 1 + NEW + n] = kt[n]
        vs = receive(4)
        ps, outs = [], []
        for n in range(NEW):
            p = reads_u[n * rows : (n + 1) * rows]
            for j in range(n):
                p = p - ps[j] * u_c[n][j] + vs[j] * u_k[n][j]
            ps.append(p)
            o_n = reads_q[n * rows : (n + 1) * rows]
            for j in range(n + 1):
                o_n = o_n - ps[j] * q_c[n][j] + vs[j] * q_k[n][j]
            mean = jnp.mean(o_n, 1, keepdims=True)
            off = o_n - mean
            var = jnp.mean(off * off, 1, keepdims=True)
            outs.append(lives[n] * (off * lax.rsqrt(var + group_epsilon) * rows_gain[b]))
        gates = receive(5)
        for n in range(NEW):
            mixrel[n] = jax.nn.sigmoid(gates[n]) * outs[n]
            for hp in range(heads // 2):
                even = mixrel[n, pl.ds(2 * hp, seqs, stride=heads), :]
                odd = mixrel[n, pl.ds(2 * hp + 1, seqs, stride=heads), :]
                mixf[hp, pl.ds(n, seqs, stride=NEW), :] = jnp.where(low, even, odd)
        for hp in range(heads // 2):
            mixed[
                b, pl.ds(pl.multiple_of(d * own, own), own), hp * LANES : (hp + 1) * LANES
            ] = mixf[hp].astype(bf16)
        mine = mixed.at[b, pl.ds(pl.multiple_of(d * own, own), own)]
        mix_copies = [
            remote(mine, mine, mix_s.at[b, o], mix_r.at[b, o], dp_peer(o)) for o in range(1, dp_n)
        ]
        for copy in mix_copies:
            copy.start()
        pending.extend(mix_copies)

        wide_lane = lax.broadcasted_iota(jnp.int32, (rows, LANES), 1) < HEAD
        for i in range(NEW):
            ship[b, 2 * i * rows : (2 * i + 1) * rows, :] = jnp.where(
                wide_lane, -ps[i], 0.0
            ).astype(bf16)
            ship[b, (2 * i + 1) * rows : (2 * i + 2) * rows, :] = jnp.where(
                wide_lane, vs[i], 0.0
            ).astype(bf16)

        new_state(b, 0, early[b])

        for copy in mix_copies:
            copy.wait_recv()
        wo_loads[b].wait()
        outp = jnp.dot(mixed[b], wo_vm[b], preferred_element_type=f32)
        psend[b] = outp.astype(bf16).reshape(2 * tp_n, half, feat)
        if b == 0:
            first = jnp.where(t >= (tp_n + 1) // 2, 1, 0)

            def pass_on(way, k, last):
                to = t + 1 - 2 * way
                back = t - 1 + 2 * way
                has_in = jnp.logical_and(back >= 0, back < tp_n)
                has_out = jnp.logical_and(to >= 0, to < tp_n)
                arrive = remote(
                    run.at[way, k], came.at[way, k], run_s.at[way, k], run_r.at[way, k], (g, t, d)
                )

                @pl.when(has_in)
                def _():
                    arrive.wait_recv()

                @pl.when(has_out)
                def _():
                    run[way, k] = (came[way, k].astype(f32) + psend[0, k].astype(f32)).astype(bf16)
                    remote(
                        run.at[way, k], came.at[way, k], run_s.at[way, k], run_r.at[way, k], (g, to, d)
                    ).start()

                if last:
                    at = pl.ds(k * half, half)
                    gat[1, at, :] = (
                        gat[0, at, :].astype(f32)
                        + (
                            psend[0, k].astype(f32)
                            + came[0, k].astype(f32)
                            + came[1, k].astype(f32)
                        )
                    ).astype(bf16)

            count = 2 * tp_n
            lag = count // 2
            for i in range(count + lag):
                if i < count:
                    pass_on(first, i, False)
                if i >= lag:
                    pass_on(1 - first, i - lag, True)
        else:
            p_copies = []
            for o in range(1, tp_n):
                copy = remote(
                    psend.at[b, pl.ds(lax.rem(t + o, tp_n) * 2, 2)],
                    precv.at[o],
                    p_s.at[o],
                    p_r.at[o],
                    tp_peer(o),
                )
                copy.start()
                p_copies.append(copy)
            pending.extend(p_copies)
            new_state(0, early[0], flat // step)
            new_state(1, early[1], flat // step)
            for m in range(2):
                rows_at = pl.ds(pl.multiple_of(t * local + m * half, half), half)
                acc = psend[b, t * 2 + m].astype(f32)
                for o in range(1, tp_n):
                    if m == 0:
                        p_copies[o - 1].wait_recv()
                    acc = acc + precv[o, m].astype(f32)
                tokens_out[m * half : (m + 1) * half, :] = (
                    gat[b, rows_at, :].astype(f32) + acc
                ).astype(bf16)

    for way in range(2):
        to = t + 1 - 2 * way

        @pl.when(jnp.logical_and(to >= 0, to < tp_n))
        def _():
            for k in range(2 * tp_n):
                remote(
                    run.at[way, k], came.at[way, k], run_s.at[way, k], run_r.at[way, k], (g, to, d)
                ).wait_send()

    for b in range(2):
        pltpu.make_async_copy(so_vm.at[b], states_out.at[b], store_sem.at[b]).wait()
    for copy in pending:
        copy.wait_send()


def solution(mesh):
    tp_n = mesh.shape["tp"]
    dp_n = mesh.shape["dp"]
    chips = dp_n // 2

    def per_device(*args):
        tokens, lengths = args[0], args[1]
        w_recept, w_out, states = args[3], args[11], args[12]
        local, feat = tokens.shape
        total = local * tp_n
        own = total // dp_n
        width = w_recept.shape[2]
        heads = width // HEAD
        seqs = lengths.shape[0]
        rows = seqs * heads
        flat = states.shape[3]
        flat_states = states.reshape(2, rows, flat)
        any_spec = pl.BlockSpec(memory_space=pl.ANY)
        hbm_spec = pl.BlockSpec(memory_space=pltpu.HBM)
        limit = 62500000
        vmem = pltpu.VMEM
        dma = pltpu.SemaphoreType.DMA
        tokens_out, states_out = pl.pallas_call(
            functools.partial(kernel, tp_n, dp_n, feat * dp_n),
            out_shape=(
                jax.ShapeDtypeStruct((local, feat), bf16),
                jax.ShapeDtypeStruct((2, rows, flat), f32),
            ),
            in_specs=[hbm_spec, pl.BlockSpec(memory_space=pltpu.SMEM)] + [hbm_spec] * 11,
            out_specs=(pl.BlockSpec(memory_space=pltpu.VMEM), any_spec),
            scratch_shapes=[
                vmem((2, total, feat), bf16),
                vmem((2, feat), f32),
                vmem((2, width), f32),
                vmem((2, width), f32),
                vmem((2, ROLES, feat, width), bf16),
                vmem((2, width, feat), bf16),
                vmem((2, rows, flat), f32),
                vmem((2, rows, flat), f32),
                vmem((flat, LANES), bf16),
                vmem((total, feat), bf16),
                vmem((2, ROLES, chips, 2, own, width), bf16),
                vmem((2, ROLES, chips, own, width), bf16),
                vmem((2, ROLES, chips, own, width), bf16),
                vmem((2, ROLES, chips, own, width), bf16),
                vmem((2, chips, 2, own, LANES), f32),
                vmem((2, chips, own, LANES), f32),
                vmem((2, chips, own, LANES), f32),
                vmem((2, chips, own, LANES), f32),
                vmem((ROLES, heads // 2, own, LANES), f32),
                vmem((ROLES * NEW, rows, LANES), f32),
                vmem((2, rows, LANES), f32),
                vmem((2, rows, LANES), f32),
                vmem((rows, LANES), f32),
                vmem((NEW * rows, flat), bf16),
                vmem((NEW, rows, LANES), f32),
                vmem((heads // 2, own, LANES), f32),
                vmem((2, total, width), bf16),
                vmem((2, 2 * tp_n, local // 2, feat), bf16),
                vmem((tp_n, 2, local // 2, feat), bf16),
                vmem((2, 2 * NEW * rows, LANES), bf16),
                vmem((2, 1 + 2 * NEW, rows, LANES), f32),
                vmem((2, 2 * tp_n, local // 2, feat), bf16),
                vmem((2, 2 * tp_n, local // 2, feat), bf16),
                dma((2, 2 * tp_n)),
                dma((2, 2 * tp_n)),
                dma((4,)),
                dma((2, ROLES + 2)),
                dma((2,)),
                dma((2, tp_n)),
                dma((2, tp_n)),
                dma((2, ROLES + 1)),
                dma((2, ROLES + 1)),
                dma((2, ROLES + 1, chips)),
                dma((2, ROLES + 1, chips)),
                dma((2, dp_n)),
                dma((2, dp_n)),
                dma((tp_n,)),
                dma((tp_n,)),
            ],
            compiler_params=pltpu.CompilerParams(
                collective_id=0, has_side_effects=True, vmem_limit_bytes=limit
            ),
        )(*args[:12], flat_states)
        return tokens_out, states_out.reshape(states.shape)

    placed = (
        P(("grp", "tp"), "dp"),
        P(("grp", "dp")),
        P(None, "dp"),
        P(None, "dp", "tp"),
        P(None, "dp", "tp"),
        P(None, "dp", "tp"),
        P(None, "dp", "tp"),
        P(None, "dp", "tp"),
        P(None, "dp", "tp"),
        P(None, "tp"),
        P(None, "tp"),
        P(None, "tp", "dp"),
        P(None, ("grp", "dp"), "tp", None),
    )
    return jax.shard_map(
        per_device,
        mesh=mesh,
        in_specs=placed,
        out_specs=(P(("grp", "tp"), "dp"), P(None, ("grp", "dp"), "tp", None)),
        check_vma=False,
    )
```

```python
import functools

import jax
import jax.numpy as jnp
from jax import lax
from jax.experimental import pallas as pl
from jax.experimental.pallas import tpu as pltpu
from jax.sharding import PartitionSpec as P

HEAD = 64
LANES = 2 * HEAD
NEW = 4
ROLES = 6
norm_epsilon = 1e-06
unit_epsilon = 0.00064
group_epsilon = 0.00064
MESH = pl.DeviceIdType.MESH
f32 = jnp.float32
bf16 = jnp.bfloat16


def kernel(
    tp_n,
    dp_n,
    model_width,
    tokens,
    lengths,
    norm_gain,
    w_recept,
    w_keys,
    w_values,
    w_decay,
    w_rate,
    w_gate,
    decay_base,
    group_gain,
    w_out,
    states,
    tokens_out,
    states_out,
    gat,
    gain_vm,
    base_vm,
    group_vm,
    w_vm,
    wo_vm,
    st_vm,
    so_vm,
    expand,
    scaled,
    part,
    pair,
    csend,
    crecv,
    sq_part,
    sq_pair,
    sq_send,
    sq_recv,
    yscr,
    rel,
    rows_base,
    rows_gain,
    rows_len,
    prod,
    mixrel,
    mixf,
    mixed,
    psend,
    precv,
    ship,
    factors,
    load_sem,
    w_sem,
    store_sem,
    gat_s,
    gat_r,
    pair_s,
    pair_r,
    cs_s,
    cs_r,
    mix_s,
    mix_r,
    p_s,
    p_r,
):
    g = lax.axis_index("grp")
    t = lax.axis_index("tp")
    d = lax.axis_index("dp")
    chips = dp_n // 2
    x = d // 2
    c = lax.rem(d, 2)
    local, feat = tokens.shape
    total = local * tp_n
    own = total // dp_n
    width = w_recept.shape[2]
    heads = width // HEAD
    seqs = own // NEW
    rows = seqs * heads
    flat = states.shape[2]

    own_gat = gat.at[0, pl.ds(pl.multiple_of(t * local, local), local)]
    loads = [
        pltpu.make_async_copy(tokens, own_gat, load_sem.at[0]),
        pltpu.make_async_copy(norm_gain, gain_vm, load_sem.at[1]),
        pltpu.make_async_copy(decay_base, base_vm, load_sem.at[2]),
        pltpu.make_async_copy(group_gain, group_vm, load_sem.at[3]),
    ]
    for copy in loads:
        copy.start()
    weights = (w_keys, w_decay, w_recept, w_rate, w_values, w_gate)
    w_loads, wo_loads, st_loads = [], [], []
    for b in range(2):
        w_loads.append(
            [
                pltpu.make_async_copy(weights[r].at[b], w_vm.at[b, r], w_sem.at[b, r])
                for r in range(ROLES)
            ]
        )
        st_loads.append(pltpu.make_async_copy(states.at[b], st_vm.at[b], w_sem.at[b, ROLES]))
        wo_loads.append(pltpu.make_async_copy(w_out.at[b], wo_vm.at[b], w_sem.at[b, ROLES + 1]))
        for copy in w_loads[b]:
            copy.start()
        st_loads[b].start()
        wo_loads[b].start()

    def tp_peer(o):
        return (g, lax.rem(t + o, tp_n), d)

    def dp_peer(o):
        return (g, t, lax.rem(d + o, dp_n))

    sibling = (g, t, x * 2 + 1 - c)

    def chip_peer(o):
        return (g, t, lax.rem(x + o, chips) * 2 + c)

    barrier = pltpu.get_barrier_semaphore()
    for o in range(1, tp_n):
        pl.semaphore_signal(barrier, inc=1, device_id=tp_peer(o), device_id_type=MESH)
    for o in range(1, dp_n):
        pl.semaphore_signal(barrier, inc=1, device_id=dp_peer(o), device_id_type=MESH)
    pl.semaphore_wait(barrier, tp_n - 1 + dp_n - 1)

    def remote(src, dst, ss, rs, dev):
        return pltpu.make_async_remote_copy(
            src_ref=src, dst_ref=dst, send_sem=ss, recv_sem=rs, device_id=dev, device_id_type=MESH
        )

    pending = []

    def gather_tokens(b):
        mine = gat.at[b, pl.ds(pl.multiple_of(t * local, local), local)]
        copies = [
            remote(mine, mine, gat_s.at[b, o], gat_r.at[b, o], tp_peer(o)) for o in range(1, tp_n)
        ]
        for copy in copies:
            copy.start()
        pending.extend(copies)
        return copies

    loads[0].wait()
    arrivals = gather_tokens(0)
    for copy in loads[1:]:
        copy.wait()

    lane = lax.broadcasted_iota(jnp.int32, (seqs, LANES), 1)
    low = lane < HEAD

    chunk = 512
    for i in range(flat // chunk):
        r_id = lax.broadcasted_iota(jnp.int32, (chunk, LANES), 0) + i * chunk
        c_id = lax.broadcasted_iota(jnp.int32, (chunk, LANES), 1)
        expand[pl.ds(i * chunk, chunk), :] = jnp.where(
            (r_id // HEAD) == lax.rem(c_id, HEAD), 1.0, 0.0
        ).astype(bf16)
    for b in range(2):
        for src, dst in ((base_vm, rows_base), (group_vm, rows_gain)):
            for hp in range(heads // 2):
                a = jnp.broadcast_to(src[b : b + 1, hp * LANES : (hp + 1) * LANES], (seqs, LANES))
                turned = pltpu.roll(a, HEAD, 1)
                dst[b, pl.ds(2 * hp, seqs, stride=heads), :] = jnp.where(low, a, turned)
                dst[b, pl.ds(2 * hp + 1, seqs, stride=heads), :] = jnp.where(low, turned, a)
    for s in range(seqs):
        rows_len[s * heads : (s + 1) * heads, :] = jnp.full(
            (heads, LANES), lengths[s].astype(f32), f32
        )

    half = local // 2
    step = 512
    early = (4, 4)

    def half_sum(z):
        return 0.5 * jnp.sum(z, 1, keepdims=True)

    def new_state(b, start, stop):
        for j in range(start, stop):
            spread = lax.dot_general(
                ship[b],
                expand[j * step : (j + 1) * step, :],
                (((1,), (1,)), ((), ())),
                preferred_element_type=f32,
            )
            for m in range(step // LANES):
                lanes = slice(m * LANES, (m + 1) * LANES)
                at = slice(j * step + m * LANES, j * step + (m + 1) * LANES)
                acc = st_vm[b, :, at] * factors[b, 0]
                for i in range(NEW):
                    acc = (
                        acc
                        + spread[2 * i * rows : (2 * i + 1) * rows, lanes] * factors[b, 1 + i]
                        + spread[(2 * i + 1) * rows : (2 * i + 2) * rows, lanes]
                        * factors[b, 1 + NEW + i]
                    )
                so_vm[b, :, at] = acc
        if stop == flat // step and start < stop:
            pltpu.make_async_copy(so_vm.at[b], states_out.at[b], store_sem.at[b]).start()

    for b in range(2):
        for copy in arrivals:
            copy.wait_recv()
        wide = gat[b].astype(f32)
        scaled[...] = (wide * gain_vm[b : b + 1, :]).astype(bf16)
        square = jnp.broadcast_to(jnp.sum(wide * wide, 1, keepdims=True), (total, LANES))
        sq_part[b] = square.reshape(chips, 2, own, LANES)

        def to_sibling(src, dst, i):
            copy = remote(
                src.at[:, 1 - c], dst, pair_s.at[b, i], pair_r.at[b, i], sibling
            )
            copy.start()
            pending.append(copy)
            return copy

        def to_chips(src, dst, i):
            copies = []
            for o in range(1, chips):
                copy = remote(
                    src.at[lax.rem(x + o, chips)],
                    dst.at[o],
                    cs_s.at[b, i, o],
                    cs_r.at[b, i, o],
                    chip_peer(o),
                )
                copy.start()
                copies.append(copy)
            pending.extend(copies)
            return copies

        pair_copies = [to_sibling(sq_part.at[b], sq_pair.at[b], ROLES)]
        chip_copies = []

        def forward_square():
            pair_copies[0].wait_recv()
            for o in range(1, chips):
                xx = lax.rem(x + o, chips)
                sq_send[b, xx] = sq_part[b, xx, c] + sq_pair[b, xx]
            chip_copies.append(to_chips(sq_send.at[b], sq_recv.at[b], ROLES))

        def forward(r):
            pair_copies[r + 1].wait_recv()
            for o in range(1, chips):
                xx = lax.rem(x + o, chips)
                csend[b, r, xx] = (
                    part[b, r, xx, c].astype(f32) + pair[b, r, xx].astype(f32)
                ).astype(bf16)
            chip_copies.append(to_chips(csend.at[b, r], crecv.at[b, r], r))

        for r in range(ROLES):
            w_loads[b][r].wait()
            y = jnp.dot(scaled[...], w_vm[b, r], preferred_element_type=f32)
            part[b, r] = y.astype(bf16).reshape(chips, 2, own, width)
            pair_copies.append(to_sibling(part.at[b, r], pair.at[b, r], r))
            if r == 0:
                forward_square()
            else:
                forward(r - 1)
        forward(ROLES - 1)

        for copy in chip_copies[0]:
            copy.wait_recv()
        square = sq_part[b, x, c] + sq_pair[b, x]
        for o in range(1, chips):
            square = square + sq_recv[b, o]
        inv_rms = lax.rsqrt(square[:, :1] / model_width + norm_epsilon)

        def receive(r):
            for copy in chip_copies[r + 1]:
                copy.wait_recv()
            y = part[b, r, x, c].astype(f32) + pair[b, r, x].astype(f32)
            for o in range(1, chips):
                y = y + crecv[b, r, o].astype(f32)
            y = (inv_rms * y).astype(bf16).astype(f32)
            for hp in range(heads // 2):
                yscr[r, hp] = y[:, hp * LANES : (hp + 1) * LANES]
            for n in range(NEW):
                for hp in range(heads // 2):
                    a = yscr[r, hp, pl.ds(n, seqs, stride=NEW), :]
                    turned = pltpu.roll(a, HEAD, 1)
                    rel[r * NEW + n, pl.ds(2 * hp, seqs, stride=heads), :] = jnp.where(
                        low, a, turned
                    )
                    rel[r * NEW + n, pl.ds(2 * hp + 1, seqs, stride=heads), :] = jnp.where(
                        low, turned, a
                    )
            return [rel[r * NEW + n] for n in range(NEW)]

        def read_state(vecs):
            for j in range(flat // LANES):
                s0 = st_vm[b, :, j * LANES : (j + 1) * LANES]
                for i, vec in enumerate(vecs):
                    prod[i * rows : (i + 1) * rows, j * LANES : (j + 1) * LANES] = (
                        s0 * vec
                    ).astype(bf16)
            return jnp.dot(prod[...], expand[...], preferred_element_type=f32)

        st_loads[b].wait()
        keys = receive(0)
        decs = receive(1)
        lives, ws, units, ks, vecs, carry = [], [], [], [], [], []
        carried = None
        for n in range(NEW):
            live = jnp.where(rows_len[...] > n + 0.5, 1.0, 0.0)
            w = jnp.exp(-jnp.exp(-jax.nn.softplus(-(rows_base[b] + decs[n])) - 0.5))
            w = jnp.where(live > 0.5, w, 1.0)
            k = keys[n]
            u = k * lax.rsqrt(half_sum(k * k) + unit_epsilon)
            lives.append(live)
            units.append(u)
            ks.append(live * k)
            ws.append(w)
            vecs.append(u if carried is None else carried * u)
            carried = w if carried is None else carried * w
            carry.append(carried)
        reads_u = read_state(vecs)
        qs = receive(2)
        reads_q = read_state([carry[n] * qs[n] for n in range(NEW)])
        rates = receive(3)
        cs = [lives[n] * (units[n] * jax.nn.sigmoid(rates[n])) for n in range(NEW)]
        ct, kt, u_c, u_k, q_c, q_k = [], [], [], [], [], []
        for n in range(NEW):
            u_c.append([half_sum(z * units[n]) for z in ct])
            u_k.append([half_sum(z * units[n]) for z in kt])
            ct = [z * ws[n] for z in ct] + [cs[n]]
            kt = [z * ws[n] for z in kt] + [ks[n]]
            q_c.append([half_sum(z * qs[n]) for z in ct])
            q_k.append([half_sum(z * qs[n]) for z in kt])
        factors[b, 0] = carried
        for n in range(NEW):
            factors[b, 1 + n] = ct[n]
            factors[b, 1 + NEW + n] = kt[n]
        vs = receive(4)
        ps, outs = [], []
        for n in range(NEW):
            p = reads_u[n * rows : (n + 1) * rows]
            for j in range(n):
                p = p - ps[j] * u_c[n][j] + vs[j] * u_k[n][j]
            ps.append(p)
            o_n = reads_q[n * rows : (n + 1) * rows]
            for j in range(n + 1):
                o_n = o_n - ps[j] * q_c[n][j] + vs[j] * q_k[n][j]
            mean = jnp.mean(o_n, 1, keepdims=True)
            off = o_n - mean
            var = jnp.mean(off * off, 1, keepdims=True)
            outs.append(lives[n] * (off * lax.rsqrt(var + group_epsilon) * rows_gain[b]))
        gates = receive(5)
        for n in range(NEW):
            mixrel[n] = jax.nn.sigmoid(gates[n]) * outs[n]
            for hp in range(heads // 2):
                even = mixrel[n, pl.ds(2 * hp, seqs, stride=heads), :]
                odd = mixrel[n, pl.ds(2 * hp + 1, seqs, stride=heads), :]
                mixf[hp, pl.ds(n, seqs, stride=NEW), :] = jnp.where(low, even, odd)
        for hp in range(heads // 2):
            mixed[
                b, pl.ds(pl.multiple_of(d * own, own), own), hp * LANES : (hp + 1) * LANES
            ] = mixf[hp].astype(bf16)
        mine = mixed.at[b, pl.ds(pl.multiple_of(d * own, own), own)]
        mix_copies = [
            remote(mine, mine, mix_s.at[b, o], mix_r.at[b, o], dp_peer(o)) for o in range(1, dp_n)
        ]
        for copy in mix_copies:
            copy.start()
        pending.extend(mix_copies)

        wide_lane = lax.broadcasted_iota(jnp.int32, (rows, LANES), 1) < HEAD
        for i in range(NEW):
            ship[b, 2 * i * rows : (2 * i + 1) * rows, :] = jnp.where(
                wide_lane, -ps[i], 0.0
            ).astype(bf16)
            ship[b, (2 * i + 1) * rows : (2 * i + 2) * rows, :] = jnp.where(
                wide_lane, vs[i], 0.0
            ).astype(bf16)

        new_state(b, 0, early[b])

        for copy in mix_copies:
            copy.wait_recv()
        wo_loads[b].wait()
        outp = jnp.dot(mixed[b], wo_vm[b], preferred_element_type=f32)
        psend[b] = outp.astype(bf16).reshape(2 * tp_n, half, feat)
        p_copies = []
        for o in range(1, tp_n):
            copy = remote(
                psend.at[b, pl.ds(lax.rem(t + o, tp_n) * 2, 2)],
                precv.at[b, o],
                p_s.at[b, o],
                p_r.at[b, o],
                tp_peer(o),
            )
            copy.start()
            p_copies.append(copy)
        pending.extend(p_copies)
        if b == 0:
            new_state(0, early[0], 8)
        else:
            new_state(0, 8, flat // step)
            new_state(1, early[1], flat // step)
        for m in range(2):
            rows_at = pl.ds(pl.multiple_of(t * local + m * half, half), half)
            acc = psend[b, t * 2 + m].astype(f32)
            for o in range(1, tp_n):
                if m == 0:
                    p_copies[o - 1].wait_recv()
                acc = acc + precv[b, o, m].astype(f32)
            fresh = (gat[b, rows_at, :].astype(f32) + acc).astype(bf16)
            if b == 0:
                gat[1, rows_at, :] = fresh
            else:
                tokens_out[m * half : (m + 1) * half, :] = fresh
        if b == 0:
            arrivals = gather_tokens(1)

    for b in range(2):
        pltpu.make_async_copy(so_vm.at[b], states_out.at[b], store_sem.at[b]).wait()
    for copy in pending:
        copy.wait_send()


def land(moved, states, moved_out, states_out, small, buf, in_sem, out_sem):
    depth = buf.shape[1]
    pieces = buf.shape[0] // 2
    pairs = [
        (
            pltpu.make_async_copy(moved, small, in_sem.at[2 * pieces]),
            pltpu.make_async_copy(small, moved_out, out_sem.at[2 * pieces]),
        )
    ]
    for b in range(2):
        for i in range(pieces):
            at = pl.ds(i * depth, depth)
            k = b * pieces + i
            pairs.append(
                (
                    pltpu.make_async_copy(states.at[b, at], buf.at[k], in_sem.at[k]),
                    pltpu.make_async_copy(buf.at[k], states_out.at[b, at], out_sem.at[k]),
                )
            )
    for come, _ in pairs:
        come.start()
    for come, go in pairs:
        come.wait()
        go.start()
    for _, go in pairs:
        go.wait()


def solution(mesh):
    tp_n = mesh.shape["tp"]
    dp_n = mesh.shape["dp"]
    chips = dp_n // 2

    def per_device(*args):
        tokens, lengths = args[0], args[1]
        w_recept, w_out, states = args[3], args[11], args[12]
        local, feat = tokens.shape
        total = local * tp_n
        own = total // dp_n
        width = w_recept.shape[2]
        heads = width // HEAD
        seqs = lengths.shape[0]
        rows = seqs * heads
        flat = states.shape[3]
        flat_states = states.reshape(2, rows, flat)
        any_spec = pl.BlockSpec(memory_space=pl.ANY)
        hbm_spec = pl.BlockSpec(memory_space=pltpu.HBM)
        limit = 62500000
        vmem = pltpu.VMEM
        dma = pltpu.SemaphoreType.DMA
        tokens_out, states_out = pl.pallas_call(
            functools.partial(kernel, tp_n, dp_n, feat * dp_n),
            out_shape=(
                jax.ShapeDtypeStruct((local, feat), bf16),
                jax.ShapeDtypeStruct((2, rows, flat), f32),
            ),
            in_specs=[hbm_spec, pl.BlockSpec(memory_space=pltpu.SMEM)] + [hbm_spec] * 11,
            out_specs=(pl.BlockSpec(memory_space=pltpu.VMEM), any_spec),
            scratch_shapes=[
                vmem((2, total, feat), bf16),
                vmem((2, feat), f32),
                vmem((2, width), f32),
                vmem((2, width), f32),
                vmem((2, ROLES, feat, width), bf16),
                vmem((2, width, feat), bf16),
                vmem((2, rows, flat), f32),
                vmem((2, rows, flat), f32),
                vmem((flat, LANES), bf16),
                vmem((total, feat), bf16),
                vmem((2, ROLES, chips, 2, own, width), bf16),
                vmem((2, ROLES, chips, own, width), bf16),
                vmem((2, ROLES, chips, own, width), bf16),
                vmem((2, ROLES, chips, own, width), bf16),
                vmem((2, chips, 2, own, LANES), f32),
                vmem((2, chips, own, LANES), f32),
                vmem((2, chips, own, LANES), f32),
                vmem((2, chips, own, LANES), f32),
                vmem((ROLES, heads // 2, own, LANES), f32),
                vmem((ROLES * NEW, rows, LANES), f32),
                vmem((2, rows, LANES), f32),
                vmem((2, rows, LANES), f32),
                vmem((rows, LANES), f32),
                vmem((NEW * rows, flat), bf16),
                vmem((NEW, rows, LANES), f32),
                vmem((heads // 2, own, LANES), f32),
                vmem((2, total, width), bf16),
                vmem((2, 2 * tp_n, local // 2, feat), bf16),
                vmem((2, tp_n, 2, local // 2, feat), bf16),
                vmem((2, 2 * NEW * rows, LANES), bf16),
                vmem((2, 1 + 2 * NEW, rows, LANES), f32),
                dma((4,)),
                dma((2, ROLES + 2)),
                dma((2,)),
                dma((2, tp_n)),
                dma((2, tp_n)),
                dma((2, ROLES + 1)),
                dma((2, ROLES + 1)),
                dma((2, ROLES + 1, chips)),
                dma((2, ROLES + 1, chips)),
                dma((2, dp_n)),
                dma((2, dp_n)),
                dma((2, tp_n)),
                dma((2, tp_n)),
            ],
            compiler_params=pltpu.CompilerParams(
                collective_id=0, has_side_effects=True, vmem_limit_bytes=limit
            ),
        )(*args[:12], flat_states)
        tokens_out, states_out = pl.pallas_call(
            land,
            out_shape=(
                jax.ShapeDtypeStruct((local, feat), bf16),
                jax.ShapeDtypeStruct((2, rows, flat), f32),
            ),
            in_specs=[any_spec] * 2,
            out_specs=(any_spec, any_spec),
            scratch_shapes=[
                vmem((local, feat), bf16),
                vmem((rows // 4, 8, flat), f32),
                dma((rows // 4 + 1,)),
                dma((rows // 4 + 1,)),
            ],
            compiler_params=pltpu.CompilerParams(vmem_limit_bytes=limit),
        )(tokens_out, states_out)
        return tokens_out, states_out.reshape(states.shape)

    placed = (
        P(("grp", "tp"), "dp"),
        P(("grp", "dp")),
        P(None, "dp"),
        P(None, "dp", "tp"),
        P(None, "dp", "tp"),
        P(None, "dp", "tp"),
        P(None, "dp", "tp"),
        P(None, "dp", "tp"),
        P(None, "dp", "tp"),
        P(None, "tp"),
        P(None, "tp"),
        P(None, "tp", "dp"),
        P(None, ("grp", "dp"), "tp", None),
    )
    return jax.shard_map(
        per_device,
        mesh=mesh,
        in_specs=placed,
        out_specs=(P(("grp", "tp"), "dp"), P(None, ("grp", "dp"), "tp", None)),
        check_vma=False,
    )
```
